32 devices in a mesh: sp: 8 (over z, y), tp: 4 (over x, core).
Axes of the slice: x: 2, y: 2, z: 4, core: 2. Of those that a mesh axis runs over, the one named last changes fastest.
Arguments:
- query_one: bfloat16 [2048, 512], P('sp', 'tp'), may hold values from -190 to 190
- query_two: bfloat16 [2048, 512], P('sp', 'tp'), may hold values from -190 to 190
- key_one: bfloat16 [2048, 512], P('sp', 'tp'), may hold values from -10 to 10
- key_two: bfloat16 [2048, 512], P('sp', 'tp'), may hold values from -10 to 10
- values: bfloat16 [2048, 1024], P('sp', 'tp'), may hold values from -6 to 6
- mix_lambda: float32 [8], P('tp'), may hold values from 0.3 to 0.8
- head_gain: float32 [128], replicated, may hold values from 0.1 to 1.9
- stream: bfloat16 [2048, 2048], P('sp', 'tp'), may hold values from -6 to 6
- out_weight: bfloat16 [1024, 2048], P('tp'), may hold values from -0.1875 to 0.1875
- first_gain: float32 [2048], replicated, may hold values from 0.1 to 1.9
- up_weight: bfloat16 [2048, 4096], P('sp', 'tp'), may hold values from -0.125 to 0.125
- down_weight: bfloat16 [4096, 2048], P('tp', 'sp'), may hold values from -0.09375 to 0.09375
- second_gain: float32 [2048], replicated, may hold values from 0.1 to 1.9
Outputs:
- layer_out: bfloat16 [2048, 2048], P(('sp', 'tp'))
The draws below stay inside these ranges and needn't reach their ends.
All inputs are finite; a program needn't handle non-finite values.
Results may differ from the reference program's by a relative error of at most 0.019.
Values may be sent and summed in bfloat16 or wider, within the bound.
No kernel may reach another device: no remote copies, remote signals or barrier semaphores. Data moves between devices by JAX's collectives and lax.ppermute only.
A program may use at most 128 MiB of HBM per device.

```python
import math
import jax
import jax.numpy as jnp
from jax import lax

D = 2048
HEADS = 8
QK = 64
VD = 128
FF = 4096
SEQ = 2048
HV = 1024


def drawn_pair(key, which):
    key_query = jax.random.fold_in(key, 11 + which)
    key_keys = jax.random.fold_in(key, 23 + which)
    width = HEADS * QK
    keys_drawn = jnp.clip(jax.random.normal(key_keys, (SEQ, width), jnp.float32), -7.0, 7.0) * 1.3
    queries = jnp.clip(jax.random.normal(key_query, (SEQ, width), jnp.float32), -7.0, 7.0) * 1.3
    return (queries, keys_drawn)


def draw_query_one(key, part):
    return drawn_pair(key, 1)[0].astype(jnp.bfloat16)


def draw_key_one(key, part):
    return drawn_pair(key, 1)[1].astype(jnp.bfloat16)


def draw_query_two(key, part):
    return drawn_pair(key, 2)[0].astype(jnp.bfloat16)


def draw_key_two(key, part):
    return drawn_pair(key, 2)[1].astype(jnp.bfloat16)


def block_scale(rng, dims, split, low, high):
    level, own = 1.0, jax.random.fold_in(rng, 6)
    for dim, blocks in split:
        heights = jnp.exp(jax.random.uniform(jax.random.fold_in(own, dim), (blocks,), jnp.float32, low / len(split), high / len(split)))
        level = level * jnp.repeat(heights, dims[dim] // blocks).reshape([-1 if axis == dim else 1 for axis in range(len(dims))])
    return level


def noise(stream_key, shape, scale, reach, cuts=(), held_as=jnp.bfloat16):
    result = scale * jax.random.normal(stream_key, shape, jnp.float32)
    if cuts:
        result = result * block_scale(stream_key, shape, cuts, -0.22, 0.18)
    return jnp.clip(result, -reach, reach).astype(held_as)


def setup_inputs(seed: int = 0) -> dict:
    key_of = jax.random.split(jax.random.key(seed), 14)
    query_one = draw_query_one(jax.random.fold_in(key_of[13], 71), 0)
    query_two = draw_query_two(jax.random.fold_in(key_of[13], 71), 0)
    key_one = draw_key_one(jax.random.fold_in(key_of[13], 71), 0)
    key_two = draw_key_two(jax.random.fold_in(key_of[13], 71), 0)
    values = noise(key_of[4], (SEQ, HV), 1.0, 6.0, ((0, 8), (1, 4)))
    mix_lambda = jnp.clip(0.3 + 0.5 * jax.random.uniform(key_of[5], (HEADS,), jnp.float32) ** block_scale(key_of[5], (HEADS,), ((0, 4),), -0.2, 0.2), 0.3, 0.8)
    head_gain = jnp.clip(1.0 + 0.18 * jax.random.normal(key_of[6], (VD,), jnp.float32), 0.1, 1.9)
    stream = noise(key_of[7], (SEQ, D), 1.0, 6.0, ((0, 8), (1, 4)))
    out_weight = noise(key_of[8], (HV, D), HV ** -0.5, 0.1875, ((0, 4),))
    first_gain = jnp.clip(1.0 + 0.18 * jax.random.normal(key_of[9], (D,), jnp.float32), 0.1, 1.9)
    up_weight = noise(key_of[10], (D, FF), D ** -0.5, 0.125, ((0, 8), (1, 4)))
    down_weight = noise(key_of[11], (FF, D), FF ** -0.5, 0.09375, ((0, 4), (1, 8)))
    second_gain = jnp.clip(1.0 + 0.18 * jax.random.normal(key_of[12], (D,), jnp.float32), 0.1, 1.9)
    return dict(query_one=query_one, query_two=query_two, key_one=key_one, key_two=key_two, values=values, mix_lambda=mix_lambda, head_gain=head_gain, stream=stream, out_weight=out_weight, first_gain=first_gain, up_weight=up_weight, down_weight=down_weight, second_gain=second_gain)


alpha_mix = 2.0 ** 0.5

def layer_norm(value, gain):
    centre = lax.optimization_barrier(jnp.mean(value, axis=-1, keepdims=True))
    spread = lax.optimization_barrier(jnp.mean(jnp.square(value - centre), axis=-1, keepdims=True))
    return (value - centre) * lax.rsqrt(spread + 1e-05) * gain

def one_map(query_blk, keys, values):
    scores = jnp.dot(query_blk, keys.T, preferred_element_type=jnp.float32) * QK ** (-0.5)
    shifted = scores - lax.optimization_barrier(jnp.max(scores, axis=-1, keepdims=True))
    expo = jnp.exp(shifted)
    total = lax.optimization_barrier(jnp.sum(expo, axis=-1, keepdims=True))
    return jnp.dot(expo.astype(jnp.bfloat16), values, preferred_element_type=jnp.float32) / total

def reference(query_one, query_two, key_one, key_two, values, mix_lambda, head_gain, stream, out_weight, first_gain, up_weight, down_weight, second_gain):

    def heads(array, width):
        return jnp.transpose(array.reshape(SEQ, HEADS, width), (1, 0, 2))
    qblk = math.gcd(SEQ, 512)
    nblk = SEQ // qblk

    def per_head(args):
        q_one, q_two, k_one, k_two, vals, weight = args
        q_one = q_one.reshape(nblk, qblk, QK)
        q_two = q_two.reshape(nblk, qblk, QK)

        def per_block(pair):
            return one_map(pair[0], k_one, vals) - weight * one_map(pair[1], k_two, vals)
        return lax.map(per_block, (q_one, q_two)).reshape(SEQ, VD)
    mixed = lax.map(per_head, (heads(query_one, QK), heads(query_two, QK), heads(key_one, QK), heads(key_two, QK), heads(values, VD), mix_lambda))
    normed = mixed * lax.rsqrt(lax.optimization_barrier(jnp.mean(jnp.square(mixed), axis=-1, keepdims=True)) + 1e-05) * head_gain * 0.8
    attended = jnp.transpose(normed.astype(jnp.bfloat16), (1, 0, 2)).reshape(SEQ, HV)
    pre = alpha_mix * stream.astype(jnp.float32) + jnp.dot(attended, out_weight, preferred_element_type=jnp.float32)
    hidden_in = layer_norm(pre, first_gain).astype(jnp.bfloat16)
    upper = jnp.dot(hidden_in, up_weight, preferred_element_type=jnp.float32)
    act = jnp.square(jax.nn.relu(upper)).astype(jnp.bfloat16)
    post = alpha_mix * hidden_in.astype(jnp.float32) + jnp.dot(act, down_weight, preferred_element_type=jnp.float32)
    return layer_norm(post, second_gain).astype(jnp.bfloat16)
```

```python
import functools
import math

import jax
import jax.numpy as jnp
from jax import lax
from jax.experimental import pallas as pl
from jax.experimental.pallas import tpu as pltpu
from jax.sharding import PartitionSpec as P

alpha_mix = 2.0**0.5
BF, F32 = jnp.bfloat16, jnp.float32


def layer_norm(value, gain):
    centre = jnp.mean(value, axis=-1, keepdims=True)
    spread = jnp.mean(jnp.square(value - centre), axis=-1, keepdims=True)
    return (value - centre) * lax.rsqrt(spread + 1e-05) * gain


def absorb_map(run_max, run_sum, run_acc, queries, keys, vals, scale):
    scores = jnp.einsum("qhd,khd->hqk", queries, keys, preferred_element_type=jnp.float32) * scale
    new_max = jnp.maximum(run_max, jnp.max(scores, axis=-1))
    factor = jnp.exp(run_max - new_max)
    expo = jnp.exp(scores - new_max[..., None])
    run_sum = run_sum * factor + jnp.sum(expo, axis=-1)
    run_acc = run_acc * factor[..., None] + jnp.einsum(
        "hqk,khe->hqe", expo.astype(jnp.bfloat16), vals, preferred_element_type=jnp.float32
    )
    return (new_max, run_sum, run_acc)


def local_general(
    query_one,
    query_two,
    key_one,
    key_two,
    values,
    mix_lambda,
    head_gain,
    stream,
    out_weight,
    first_gain,
    up_weight,
    down_weight,
    second_gain,
):
    tokens = query_one.shape[0]
    heads_local = mix_lambda.shape[0]
    qk_width = query_one.shape[1] // heads_local
    v_width = values.shape[1] // heads_local
    scale = qk_width ** (-0.5)
    queries_a = query_one.reshape(tokens, heads_local, qk_width)
    queries_b = query_two.reshape(tokens, heads_local, qk_width)
    lowest = jnp.full((heads_local, tokens), -1e30, jnp.float32)
    zero_sum = jnp.zeros((heads_local, tokens), jnp.float32)
    zero_acc = jnp.zeros((heads_local, tokens, v_width), jnp.float32)
    pieces = (
        lax.all_gather(key_one, "sp", axis=0, tiled=True),
        lax.all_gather(key_two, "sp", axis=0, tiled=True),
        lax.all_gather(values, "sp", axis=0, tiled=True),
    )
    count = pieces[0].shape[0]
    block = math.gcd(count, 1024)
    nblk = count // block
    keys_a = pieces[0].reshape(nblk, block, heads_local, qk_width)
    keys_b = pieces[1].reshape(nblk, block, heads_local, qk_width)
    vals = pieces[2].reshape(nblk, block, heads_local, v_width)

    def step(carry, inputs):
        max_a, sum_a, acc_a, max_b, sum_b, acc_b = carry
        max_a, sum_a, acc_a = absorb_map(
            max_a, sum_a, acc_a, queries_a, inputs[0], inputs[2], scale
        )
        max_b, sum_b, acc_b = absorb_map(
            max_b, sum_b, acc_b, queries_b, inputs[1], inputs[2], scale
        )
        return ((max_a, sum_a, acc_a, max_b, sum_b, acc_b), None)

    result, _ = lax.scan(
        step, (lowest, zero_sum, zero_acc, lowest, zero_sum, zero_acc), (keys_a, keys_b, vals)
    )
    max_a, sum_a, acc_a, max_b, sum_b, acc_b = result
    mixed = acc_a / sum_a[..., None] - mix_lambda[:, None, None] * acc_b / sum_b[..., None]
    normed = (
        mixed
        * lax.rsqrt(jnp.mean(jnp.square(mixed), axis=-1, keepdims=True) + 1e-05)
        * head_gain
        * 0.8
    )
    attended = jnp.transpose(normed.astype(jnp.bfloat16), (1, 0, 2)).reshape(
        tokens, heads_local * v_width
    )
    tp_index = lax.axis_index("tp")
    own_cols = stream.shape[1]
    col_start = tp_index * own_cols
    share = tokens // lax.axis_size("tp")
    row_start = tp_index * share
    partial_rows = jnp.dot(attended, out_weight, preferred_element_type=jnp.float32)
    own = lax.dynamic_slice_in_dim(partial_rows, col_start, own_cols, 1)
    own = own + alpha_mix * stream.astype(jnp.float32)
    pre = lax.psum(
        lax.dynamic_update_slice_in_dim(partial_rows, own, col_start, 1).astype(jnp.bfloat16), "tp"
    ).astype(jnp.float32)
    hidden_in = layer_norm(pre, first_gain).astype(jnp.bfloat16)
    up_full, down_full = (
        lax.all_gather(up_weight, "sp", axis=0, tiled=True),
        lax.all_gather(down_weight, "sp", axis=1, tiled=True),
    )
    upper = jnp.dot(hidden_in, up_full, preferred_element_type=jnp.float32)
    act = jnp.square(jax.nn.relu(upper)).astype(jnp.bfloat16)
    post = lax.psum_scatter(
        jnp.dot(act, down_full, preferred_element_type=jnp.float32).astype(jnp.bfloat16),
        "tp",
        scatter_dimension=0,
        tiled=True,
    ).astype(jnp.float32)
    post = post + alpha_mix * lax.dynamic_slice_in_dim(hidden_in, row_start, share, 0).astype(
        jnp.float32
    )
    return layer_norm(post, second_gain).astype(jnp.bfloat16)


VM = pl.BlockSpec(memory_space=pltpu.VMEM)
SM = pl.BlockSpec(memory_space=pltpu.SMEM)


def place():
    s, t = lax.axis_index("sp"), lax.axis_index("tp")
    return lax.div(s, 2), lax.rem(s, 2), lax.div(t, 2), lax.rem(t, 2)


def call(body, outs, args, specs=None, scratch=(), flops=0, name=None):
    outs = [jax.ShapeDtypeStruct(shape, kind) for shape, kind in outs]
    size = sum(a.size * a.dtype.itemsize for a in list(args) + outs)
    return pl.pallas_call(
        body,
        out_shape=outs,
        in_specs=specs or [VM] * len(args),
        out_specs=[VM] * len(outs),
        scratch_shapes=list(scratch),
        cost_estimate=pl.CostEstimate(flops=flops, bytes_accessed=size, transcendentals=0),
        name=name,
    )(*args)


def either(bit, emit):
    @pl.when(bit == 0)
    def _():
        emit(0)

    @pl.when(bit != 0)
    def _():
        emit(1)


def pack_heads(q1, q2, k1, k2, v, kv_own, kv_out, kvq_out, q_own):
    _, y, _, _ = place()
    w, e = q1.shape[1] // 2, v.shape[1] // 2

    def emit(bit):
        for head, dests in ((bit, (kv_own,)), (1 - bit, (kv_out, kvq_out))):
            for dest in dests:
                dest[:, :w] = k1[:, head * w : (head + 1) * w]
                dest[:, w : 2 * w] = k2[:, head * w : (head + 1) * w]
                dest[:, 2 * w : 2 * w + e] = v[:, head * e : (head + 1) * e]
        q_own[:, :w] = q1[:, bit * w : (bit + 1) * w]
        q_own[:, w:] = q2[:, bit * w : (bit + 1) * w]
        other, base = 1 - bit, 2 * w + e
        kvq_out[:, base : base + w] = q1[:, other * w : (other + 1) * w]
        kvq_out[:, base + w :] = q2[:, other * w : (other + 1) * w]

    either(y, emit)


def pack_weights(up, down, own, out):
    _, y, _, _ = place()
    rows, half = up.shape[0], up.shape[1] // 2
    cols, part = down.shape[1], half // 2

    def emit(bit):
        for side, dest in ((bit, own), (1 - bit, out)):
            dest[:rows, :] = up[:, side * half : (side + 1) * half]
            for k in range(2):
                first = side * half + k * part
                dest[rows:, k * cols : (k + 1) * cols] = down[first : first + part, :]

    either(y, emit)


def attention(qk, lam, gain, q_own, *refs):
    kvs, att = refs[:-1], refs[-1]
    _, y, _, _ = place()
    tokens = q_own.shape[0]
    w2 = 2 * qk
    e = att.shape[1]
    rate = qk**-0.5 * math.log2(math.e)
    lane = lax.broadcasted_iota(jnp.int32, (tokens, w2), 1)
    weight = lam[y]
    for part in range(2):
        queries = (q_own[...] if part == 0 else kvs[1][:, w2 + e :]).astype(F32)
        outs = []
        for which in range(2):
            keep = (lane < qk) if which == 0 else (lane >= qk)
            masked = jnp.where(keep, queries, 0.0).astype(BF)
            tiles = [
                lax.dot_general(
                    masked, kv[:, :w2], (((1,), (1,)), ((), ())), preferred_element_type=F32
                )
                for kv in kvs
            ]
            top = functools.reduce(jnp.maximum, tiles)
            top = jnp.max(top, axis=1, keepdims=True)
            total, acc = None, None
            for tile, kv in zip(tiles, kvs):
                expo = jnp.exp2((tile - top) * rate)
                total = expo if total is None else total + expo
                part_acc = jnp.dot(
                    expo.astype(BF), kv[:, w2 : w2 + e], preferred_element_type=F32
                )
                acc = part_acc if acc is None else acc + part_acc
            outs.append(acc / jnp.sum(total, axis=1, keepdims=True))
        mixed = outs[0] - weight * outs[1]
        normed = (
            mixed
            * lax.rsqrt(jnp.mean(jnp.square(mixed), axis=-1, keepdims=True) + 1e-05)
            * gain[...]
            * 0.8
        )
        row = (y if part == 0 else 1 - y) * tokens
        att[pl.ds(pl.multiple_of(row, tokens), tokens), :] = normed.astype(BF)


def merge_heads(a, ax, ay, axy, out):
    _, y, _, _ = place()
    e = a.shape[1]

    def emit(bit):
        for dx, pair in enumerate(((a, ay), (ax, axy))):
            for dy in range(2):
                k = dx * 2 + (bit ^ dy)
                out[:, k * e : (k + 1) * e] = pair[dy][...]

    either(y, emit)


def norm_in(a0, a1, w00, w10, w01, w11, s00, s10, s01, s11, gain, hidden):
    _, y, x, c = place()
    rows = s00.shape[0] // 2
    cols = s00.shape[1]
    depth = w00.shape[0]
    for part in range(2):
        row = pl.multiple_of((y if part == 0 else 1 - y) * rows, rows)
        left = [a0[pl.ds(row, rows), :depth], a0[pl.ds(row, rows), depth:]]
        left += [a1[pl.ds(row, rows), :depth], a1[pl.ds(row, rows), depth:]]
        groups = []
        for dx, dc, st in ((0, 0, s00), (1, 0, s10), (0, 1, s01), (1, 1, s11)):
            col = ((x ^ dx) * 2 + (c ^ dc)) * cols
            where = pl.ds(pl.multiple_of(col, cols), cols)
            acc = alpha_mix * st[part * rows : (part + 1) * rows, :].astype(F32)
            for lhs, wt in zip(left, (w00, w10, w01, w11)):
                acc = acc + jnp.dot(lhs, wt[:, where], preferred_element_type=F32)
            groups.append((where, acc))
        width = cols * len(groups)
        centre = sum(jnp.sum(g, axis=1, keepdims=True) for _, g in groups) / width
        spread = (
            sum(jnp.sum(jnp.square(g - centre), axis=1, keepdims=True) for _, g in groups) / width
        )
        factor = lax.rsqrt(spread + 1e-05)
        for where, g in groups:
            hidden[pl.ds(row, rows), where] = ((g - centre) * factor * gain[:, where]).astype(BF)


def blocks_of(refs, z):
    own, plus, minus, two, far = refs
    return (
        (lambda part: own[part], z),
        (lambda part: jnp.where(z == 0, far[part], plus[part]), lax.rem(z + 3, 4)),
        (lambda part: jnp.where(z == 3, far[part], minus[part]), lax.rem(z + 1, 4)),
        (lambda part: two[part], lax.rem(z + 2, 4)),
    )


def mixer_up(hidden, own, plus, minus, two, far, act, full):
    z, y, _, _ = place()
    rows = own.shape[1]
    for load, zz in blocks_of((own, plus, minus, two, far), z):
        for part in range(2):
            first = (2 * zz + (y ^ part)) * rows
            full[pl.ds(pl.multiple_of(first, rows), rows), :] = load(part)
    upper = jnp.dot(hidden[...], full[...], preferred_element_type=F32)
    act[...] = jnp.square(jnp.maximum(upper, 0.0)).astype(BF)


def mixer_down(act, own, plus, minus, two, far, keep, send):
    z, y, _, c = place()
    cols = own.shape[2] // 2
    share = keep.shape[1]
    for load, zz in blocks_of((own, plus, minus, two, far), z):
        for part in range(2):
            block = load(part)
            weight = jnp.concatenate([block[:, :cols], block[:, cols:]], axis=0)
            rows = jnp.dot(act[...], weight, preferred_element_type=F32)
            first = (2 * zz + (y ^ part)) * cols
            where = pl.ds(pl.multiple_of(first, cols), cols)

            def emit(bit, rows=rows, where=where):
                for k in range(keep.shape[0] * 2):
                    piece = rows[k * share : (k + 1) * share, :]
                    if k % 2 == bit:
                        keep[k // 2, :, where] = piece
                    else:
                        send[k // 2, :, where] = piece.astype(BF)

            either(c, emit)


def pair_sum(keep, got, own, to_x, to_y, to_xy):
    _, y, x, _ = place()

    def total(dy, dx):
        k = (y ^ dy) * 2 + (x ^ dx)
        return keep[k] + got[k].astype(F32)

    own[...] = total(0, 0)
    to_x[...] = total(0, 1).astype(BF)
    to_y[...] = total(1, 0).astype(BF)
    to_xy[...] = total(1, 1).astype(BF)


def norm_out(own, from_x, from_y, from_xy, hidden, gain, out):
    _, y, x, c = place()
    share = own.shape[0]
    first = ((y * 2 + x) * 2 + c) * share
    mine = hidden[pl.ds(pl.multiple_of(first, share), share), :].astype(F32)
    post = own[...] + from_x[...].astype(F32) + (from_y[...].astype(F32) + from_xy[...].astype(F32))
    out[...] = layer_norm(post + alpha_mix * mine, gain[...]).astype(BF)


def local_planes(
    query_one,
    query_two,
    key_one,
    key_two,
    values,
    mix_lambda,
    head_gain,
    stream,
    out_weight,
    first_gain,
    up_weight,
    down_weight,
    second_gain,
):
    tokens, w2 = query_one.shape
    qk = w2 // 2
    e = values.shape[1] // 2
    width = out_weight.shape[1]
    rows, half = up_weight.shape[0], up_weight.shape[1] // 2
    cols = down_weight.shape[1]

    def permute(value, move):
        pairs = []
        for z in range(4):
            for y in range(2):
                for x in range(2):
                    for c in range(2):
                        to = move(z, y, x, c)
                        if to is not None:
                            zz, yy, xx, cc = to
                            pairs.append(
                                (((z * 2 + y) * 2 + x) * 2 + c, ((zz * 2 + yy) * 2 + xx) * 2 + cc)
                            )
        return lax.ppermute(value, ("sp", "tp"), pairs)

    def across(value, dy, dx, dc):
        return permute(value, lambda z, y, x, c: (z, y ^ dy, x ^ dx, c ^ dc))

    def planes(block):
        plus = permute(block, lambda z, y, x, c: (z + 1, y, x, c) if z < 3 else None)
        minus = permute(block, lambda z, y, x, c: (z - 1, y, x, c) if z > 0 else None)
        two = permute(block, lambda z, y, x, c: ((z + 2) % 4, y, x, c))
        far = permute(
            two, lambda z, y, x, c: {1: (0, y, x, c), 2: (3, y, x, c)}.get(z)
        )
        return block, plus, minus, two, far

    kv_own, kv_out, kvq_out, q_own = call(
        pack_heads,
        [
            ((tokens, w2 + e), BF),
            ((tokens, w2 + e), BF),
            ((tokens, 2 * w2 + e), BF),
            ((tokens, w2), BF),
        ],
        (query_one, query_two, key_one, key_two, values),
        name="pack_heads",
    )
    wt_own, wt_out = call(
        pack_weights,
        [((2 * rows, half), BF)] * 2,
        (up_weight, down_weight),
        name="pack_weights",
    )
    wo_x = across(out_weight, 0, 1, 0)
    kvs = [kv_own, across(kvq_out, 1, 0, 0)]
    for dz in (1, 3, 2):
        for dy in range(2):
            kvs.append(
                permute(
                    kv_out if dy else kv_own,
                    lambda z, y, x, c, dz=dz, dy=dy: ((z + dz) % 4, y ^ dy, x, c),
                )
            )
    wt_got = across(wt_out, 1, 0, 0)
    st_y = across(stream, 1, 0, 0)
    up_blocks = planes(jnp.stack([wt_own[:rows], wt_got[:rows]]))
    down_blocks = planes(jnp.stack([wt_own[rows:], wt_got[rows:]]))
    st00 = jnp.concatenate([stream, st_y], axis=0)
    st10 = across(st00, 0, 1, 0)
    wo_c, wo_xc = across(out_weight, 0, 0, 1), across(wo_x, 0, 0, 1)
    st01, st11 = across(st00, 0, 0, 1), across(st10, 0, 0, 1)

    (att,) = call(
        functools.partial(attention, qk),
        [((2 * tokens, e), BF)],
        (mix_lambda, head_gain.reshape(1, -1), q_own, *kvs),
        specs=[SM] + [VM] * (2 + len(kvs)),
        flops=4 * 2 * tokens * tokens * len(kvs) * (qk + e),
        name="attention",
    )
    att_x, att_y, att_xy = across(att, 0, 1, 0), across(att, 1, 0, 0), across(att, 1, 1, 0)
    (heads0,) = call(
        merge_heads, [((2 * tokens, 4 * e), BF)], (att, att_x, att_y, att_xy), name="merge_heads"
    )
    heads1 = across(heads0, 0, 0, 1)
    (hidden,) = call(
        norm_in,
        [((2 * tokens, width), BF)],
        (
            heads0,
            heads1,
            out_weight,
            wo_x,
            wo_c,
            wo_xc,
            st00,
            st10,
            st01,
            st11,
            first_gain.reshape(1, -1),
        ),
        flops=2 * 2 * tokens * width * 8 * e,
        name="norm_in",
    )
    (act,) = call(
        mixer_up,
        [((2 * tokens, half), BF)],
        (hidden, *up_blocks),
        scratch=[pltpu.VMEM((8 * rows, half), BF)],
        flops=4 * tokens * width * half,
        name="mixer_up",
    )
    share = tokens // 4
    keep, send = call(
        mixer_down,
        [((4, share, width), F32), ((4, share, width), BF)],
        (act, *down_blocks),
        flops=4 * tokens * width * half,
        name="mixer_down",
    )
    got = across(send, 0, 0, 1)
    own, to_x, to_y, to_xy = call(
        pair_sum,
        [((share, width), F32)] + [((share, width), BF)] * 3,
        (keep, got),
        name="pair_sum",
    )
    from_x, from_y, from_xy = (
        across(to_x, 0, 1, 0),
        across(to_y, 1, 0, 0),
        across(to_xy, 1, 1, 0),
    )
    (out,) = call(
        norm_out,
        [((share, width), BF)],
        (own, from_x, from_y, from_xy, hidden, second_gain.reshape(1, -1)),
        name="norm_out",
    )
    return out


def solution(mesh):
    in_specs = (
        P("sp", "tp"),
        P("sp", "tp"),
        P("sp", "tp"),
        P("sp", "tp"),
        P("sp", "tp"),
        P("tp"),
        P(),
        P("sp", "tp"),
        P("tp", None),
        P(),
        P("sp", "tp"),
        P("tp", "sp"),
        P(),
    )
    out_specs = P(("sp", "tp"), None)
    planes = mesh.shape["sp"] == 8 and mesh.shape["tp"] == 4

    def local(*args):
        return (local_planes if planes and args[5].shape[0] == 2 else local_general)(*args)

    return jax.shard_map(local, mesh=mesh, in_specs=in_specs, out_specs=out_specs, check_vma=False)
```

```python
import functools
import math

import jax
import jax.numpy as jnp
from jax import lax
from jax.experimental import pallas as pl
from jax.experimental.pallas import tpu as pltpu
from jax.sharding import PartitionSpec as P


alpha_mix = 2.0**0.5
BF, F32 = jnp.bfloat16, jnp.float32


def layer_norm(value, gain):
    centre = jnp.mean(value, axis=-1, keepdims=True)
    spread = jnp.mean(jnp.square(value - centre), axis=-1, keepdims=True)
    return (value - centre) * lax.rsqrt(spread + 1e-05) * gain


def absorb_map(run_max, run_sum, run_acc, queries, keys, vals, scale):
    scores = jnp.einsum("qhd,khd->hqk", queries, keys, preferred_element_type=jnp.float32) * scale
    new_max = jnp.maximum(run_max, jnp.max(scores, axis=-1))
    factor = jnp.exp(run_max - new_max)
    expo = jnp.exp(scores - new_max[..., None])
    run_sum = run_sum * factor + jnp.sum(expo, axis=-1)
    run_acc = run_acc * factor[..., None] + jnp.einsum(
        "hqk,khe->hqe", expo.astype(jnp.bfloat16), vals, preferred_element_type=jnp.float32
    )
    return (new_max, run_sum, run_acc)


def local_general(
    query_one,
    query_two,
    key_one,
    key_two,
    values,
    mix_lambda,
    head_gain,
    stream,
    out_weight,
    first_gain,
    up_weight,
    down_weight,
    second_gain,
):
    tokens = query_one.shape[0]
    heads_local = mix_lambda.shape[0]
    qk_width = query_one.shape[1] // heads_local
    v_width = values.shape[1] // heads_local
    scale = qk_width ** (-0.5)
    queries_a = query_one.reshape(tokens, heads_local, qk_width)
    queries_b = query_two.reshape(tokens, heads_local, qk_width)
    lowest = jnp.full((heads_local, tokens), -1e30, jnp.float32)
    zero_sum = jnp.zeros((heads_local, tokens), jnp.float32)
    zero_acc = jnp.zeros((heads_local, tokens, v_width), jnp.float32)
    pieces = (
        lax.all_gather(key_one, "sp", axis=0, tiled=True),
        lax.all_gather(key_two, "sp", axis=0, tiled=True),
        lax.all_gather(values, "sp", axis=0, tiled=True),
    )
    count = pieces[0].shape[0]
    block = math.gcd(count, 1024)
    nblk = count // block
    keys_a = pieces[0].reshape(nblk, block, heads_local, qk_width)
    keys_b = pieces[1].reshape(nblk, block, heads_local, qk_width)
    vals = pieces[2].reshape(nblk, block, heads_local, v_width)

    def step(carry, inputs):
        max_a, sum_a, acc_a, max_b, sum_b, acc_b = carry
        max_a, sum_a, acc_a = absorb_map(
            max_a, sum_a, acc_a, queries_a, inputs[0], inputs[2], scale
        )
        max_b, sum_b, acc_b = absorb_map(
            max_b, sum_b, acc_b, queries_b, inputs[1], inputs[2], scale
        )
        return ((max_a, sum_a, acc_a, max_b, sum_b, acc_b), None)

    result, _ = lax.scan(
        step, (lowest, zero_sum, zero_acc, lowest, zero_sum, zero_acc), (keys_a, keys_b, vals)
    )
    _, sum_a, acc_a, _, sum_b, acc_b = result
    mixed = acc_a / sum_a[..., None] - mix_lambda[:, None, None] * acc_b / sum_b[..., None]
    normed = (
        mixed
        * lax.rsqrt(jnp.mean(jnp.square(mixed), axis=-1, keepdims=True) + 1e-05)
        * head_gain
        * 0.8
    )
    attended = jnp.transpose(normed.astype(jnp.bfloat16), (1, 0, 2)).reshape(
        tokens, heads_local * v_width
    )
    tp_index = lax.axis_index("tp")
    own_cols = stream.shape[1]
    col_start = tp_index * own_cols
    share = tokens // lax.axis_size("tp")
    row_start = tp_index * share
    partial_rows = jnp.dot(attended, out_weight, preferred_element_type=jnp.float32)
    own = lax.dynamic_slice_in_dim(partial_rows, col_start, own_cols, 1)
    own = own + alpha_mix * stream.astype(jnp.float32)
    pre = lax.psum(
        lax.dynamic_update_slice_in_dim(partial_rows, own, col_start, 1).astype(jnp.bfloat16), "tp"
    ).astype(jnp.float32)
    hidden_in = layer_norm(pre, first_gain).astype(jnp.bfloat16)
    up_full, down_full = (
        lax.all_gather(up_weight, "sp", axis=0, tiled=True),
        lax.all_gather(down_weight, "sp", axis=1, tiled=True),
    )
    upper = jnp.dot(hidden_in, up_full, preferred_element_type=jnp.float32)
    act = jnp.square(jax.nn.relu(upper)).astype(jnp.bfloat16)
    post = lax.psum_scatter(
        jnp.dot(act, down_full, preferred_element_type=jnp.float32).astype(jnp.bfloat16),
        "tp",
        scatter_dimension=0,
        tiled=True,
    ).astype(jnp.float32)
    post = post + alpha_mix * lax.dynamic_slice_in_dim(hidden_in, row_start, share, 0).astype(
        jnp.float32
    )
    return layer_norm(post, second_gain).astype(jnp.bfloat16)


VM = pl.BlockSpec(memory_space=pltpu.VMEM)
SM = pl.BlockSpec(memory_space=pltpu.SMEM)


def place():
    s, t = lax.axis_index("sp"), lax.axis_index("tp")
    return lax.div(s, 2), lax.rem(s, 2), lax.div(t, 2), lax.rem(t, 2)


def call(body, outs, args, specs=None, scratch=(), flops=0, vmem=24):
    outs = [jax.ShapeDtypeStruct(shape, kind) for shape, kind in outs]
    size = sum(a.size * a.dtype.itemsize for a in list(args) + outs)
    return pl.pallas_call(
        body,
        out_shape=outs,
        in_specs=specs or [VM] * len(args),
        out_specs=[VM] * len(outs),
        scratch_shapes=list(scratch),
        cost_estimate=pl.CostEstimate(flops=flops, bytes_accessed=size, transcendentals=0),
        compiler_params=pltpu.CompilerParams(vmem_limit_bytes=vmem * 2**20),
    )(*args)


def either(bit, emit):
    @pl.when(bit == 0)
    def _():
        emit(0)

    @pl.when(bit != 0)
    def _():
        emit(1)


def pack(q1, q2, k1, k2, v, up, down, kv_own, kv_out, kvq_out, q_own, wt_own, wt_out, *scratch):
    bufs, sems = scratch[:-1], scratch[-1]
    copies = [
        pltpu.make_async_copy(src, buf, sems.at[i])
        for i, (src, buf) in enumerate(zip((q1, q2, k1, k2, v, up, down), bufs))
    ]
    for copy in copies:
        copy.start()
    q1, q2, k1, k2, v, up, down = bufs
    _, y, _, _ = place()
    w, e = q1.shape[1] // 2, v.shape[1] // 2
    rows, half = up.shape[0], up.shape[1] // 2
    cols, part = down.shape[1], half // 2
    for copy in copies[:5]:
        copy.wait()

    def heads(bit):
        for head, dests in ((bit, (kv_own,)), (1 - bit, (kv_out, kvq_out))):
            for dest in dests:
                dest[:, :w] = k1[:, head * w : (head + 1) * w]
                dest[:, w : 2 * w] = k2[:, head * w : (head + 1) * w]
                dest[:, 2 * w : 2 * w + e] = v[:, head * e : (head + 1) * e]
        q_own[:, :w] = q1[:, bit * w : (bit + 1) * w]
        q_own[:, w:] = q2[:, bit * w : (bit + 1) * w]
        other, base = 1 - bit, 2 * w + e
        kvq_out[:, base : base + w] = q1[:, other * w : (other + 1) * w]
        kvq_out[:, base + w :] = q2[:, other * w : (other + 1) * w]

    def weights(bit):
        for side, dest in ((bit, wt_own), (1 - bit, wt_out)):
            dest[:rows, :] = up[:, side * half : (side + 1) * half]
            for k in range(2):
                first = side * half + k * part
                dest[rows:, k * cols : (k + 1) * cols] = down[first : first + part, :]

    either(y, heads)
    for copy in copies[5:]:
        copy.wait()
    either(y, weights)


def stack_weights(own, got, up, down):
    rows = up.shape[1]
    for k, src in enumerate((own, got)):
        up[k] = src[:rows, :]
        down[k] = src[rows:, :]


def stack_rows(own, got, out):
    rows = own.shape[0]
    out[:rows, :] = own[...]
    out[rows:, :] = got[...]


def attention(qk, lam, gain, q_own, *refs):
    kv_own, kvq_y = refs[:2]
    att, full = refs[10:]
    z, y, _, _ = place()
    tokens = q_own.shape[0]
    parts = [kv_own[...], kvq_y[:, : full.shape[1]]]
    for plus, minus, two, far in (refs[2:6], refs[6:10]):
        parts.append(two[...])
        parts.append(jnp.where(z == 0, far[...], plus[...]))
        parts.append(jnp.where(z == 3, far[...], minus[...]))
    for i, block in enumerate(parts):
        full[i * tokens : (i + 1) * tokens, :] = block
    kvs = [full.at[i * tokens : (i + 1) * tokens, :] for i in range(len(parts))]
    w2 = 2 * qk
    e = att.shape[1]
    rate = qk**-0.5 * math.log2(math.e)
    lane = lax.broadcasted_iota(jnp.int32, (tokens, w2), 1)
    weight = lam[y]
    for part in range(2):
        queries = (q_own[...] if part == 0 else kvq_y[:, w2 + e :]).astype(F32)
        outs = []
        for which in range(2):
            keep = (lane < qk) if which == 0 else (lane >= qk)
            masked = jnp.where(keep, queries, 0.0).astype(BF)
            tiles = [
                lax.dot_general(
                    masked, kv[:, :w2], (((1,), (1,)), ((), ())), preferred_element_type=F32
                )
                for kv in kvs
            ]
            top = functools.reduce(jnp.maximum, tiles)
            top = jnp.max(top, axis=1, keepdims=True)
            total, acc = None, None
            for tile, kv in zip(tiles, kvs):
                expo = jnp.exp2((tile - top) * rate)
                total = expo if total is None else total + expo
                part_acc = jnp.dot(
                    expo.astype(BF), kv[:, w2 : w2 + e], preferred_element_type=F32
                )
                acc = part_acc if acc is None else acc + part_acc
            outs.append(acc / jnp.sum(total, axis=1, keepdims=True))
        mixed = outs[0] - weight * outs[1]
        normed = (
            mixed
            * lax.rsqrt(jnp.mean(jnp.square(mixed), axis=-1, keepdims=True) + 1e-05)
            * gain[...]
            * 0.8
        )
        row = (y if part == 0 else 1 - y) * tokens
        att[pl.ds(pl.multiple_of(row, tokens), tokens), :] = normed.astype(BF)


def merge_heads(a, ax, ay, axy, out):
    _, y, _, _ = place()
    e = a.shape[1]

    def emit(bit):
        for dx, pair in enumerate(((a, ay), (ax, axy))):
            for dy in range(2):
                k = dx * 2 + (bit ^ dy)
                out[:, k * e : (k + 1) * e] = pair[dy][...]

    either(y, emit)


def norm_in(a0, a1, w00, w10, w01, w11, s00, s10, s01, s11, gain, hidden):
    _, y, x, c = place()
    rows = s00.shape[0] // 2
    cols = s00.shape[1]
    depth = w00.shape[0]
    for part in range(2):
        row = pl.multiple_of((y if part == 0 else 1 - y) * rows, rows)
        left = [a0[pl.ds(row, rows), :depth], a0[pl.ds(row, rows), depth:]]
        left += [a1[pl.ds(row, rows), :depth], a1[pl.ds(row, rows), depth:]]
        groups = []
        for dx, dc, st in ((0, 0, s00), (1, 0, s10), (0, 1, s01), (1, 1, s11)):
            col = ((x ^ dx) * 2 + (c ^ dc)) * cols
            where = pl.ds(pl.multiple_of(col, cols), cols)
            acc = alpha_mix * st[part * rows : (part + 1) * rows, :].astype(F32)
            for lhs, wt in zip(left, (w00, w10, w01, w11)):
                acc = acc + jnp.dot(lhs, wt[:, where], preferred_element_type=F32)
            groups.append((where, acc))
        width = cols * len(groups)
        centre = sum(jnp.sum(g, axis=1, keepdims=True) for _, g in groups) / width
        spread = (
            sum(jnp.sum(jnp.square(g - centre), axis=1, keepdims=True) for _, g in groups) / width
        )
        factor = lax.rsqrt(spread + 1e-05)
        for where, g in groups:
            hidden[pl.ds(row, rows), where] = ((g - centre) * factor * gain[:, where]).astype(BF)


def near_far(refs, z):
    own, plus, minus, two, far = refs
    return (
        (lambda part: own[part], z),
        (lambda part: two[part], lax.rem(z + 2, 4)),
        (
            lambda part: jnp.where(z == 0, minus[part], plus[part]),
            jnp.where(z == 0, 1, z - 1),
        ),
        (
            lambda part: jnp.where((z == 0) | (z == 3), far[part], minus[part]),
            jnp.where(z == 0, 3, lax.rem(z + 1, 4)),
        ),
    )


def slot_planes(z):
    return z, lax.rem(z + 2, 4), jnp.where(z == 0, 1, z - 1), jnp.where(z == 0, 3, lax.rem(z + 1, 4))


def mixer_up(hidden, own, plus, minus, two, far, act, full):
    z, y, _, _ = place()
    rows = own.shape[1]
    for load, zz in near_far((own, plus, minus, two, far), z):
        for part in range(2):
            first = (2 * zz + (y ^ part)) * rows
            full[pl.ds(pl.multiple_of(first, rows), rows), :] = load(part)
    upper = jnp.dot(hidden[...], full[...], preferred_element_type=F32)
    act[...] = jnp.square(jnp.maximum(upper, 0.0)).astype(BF)


def mixer_down(loads, act, keep, send):
    _, y, _, c = place()
    share = keep.shape[1]
    for slot, load in enumerate(loads):
        for part in range(2):
            block = load(part)
            cols = block.shape[1] // 2
            weight = jnp.concatenate([block[:, :cols], block[:, cols:]], axis=0)
            rows = jnp.dot(act[...], weight, preferred_element_type=F32)
            where = pl.ds(pl.multiple_of((2 * slot + (y ^ part)) * cols, cols), cols)

            def emit(bit, rows=rows, where=where):
                for k in range(keep.shape[0] * 2):
                    piece = rows[k * share : (k + 1) * share, :]
                    if k % 2 == bit:
                        keep[k // 2, :, where] = piece
                    else:
                        send[k // 2, :, where] = piece.astype(BF)

            either(c, emit)


def mixer_down_a(act, own, plus, minus, two, keep, send):
    z = place()[0]
    slots = near_far((own, plus, minus, two, None), z)
    mixer_down([load for load, _ in slots[:3]], act, keep, send)


def mixer_down_b(act, minus, far, keep, send):
    z = place()[0]
    slots = near_far((None, None, minus, None, far), z)
    mixer_down([load for load, _ in slots[3:]], act, keep, send)


def pair_sum(keep, got, own, to_x, to_y, to_xy):
    _, y, x, _ = place()

    def total(dy, dx):
        k = (y ^ dy) * 2 + (x ^ dx)
        return keep[k] + got[k].astype(F32)

    to_x[...] = total(0, 1).astype(BF)
    to_y[...] = total(1, 0).astype(BF)
    to_xy[...] = total(1, 1).astype(BF)
    own[...] = total(0, 0)


def norm_out(*refs):
    parts, (hidden, gain, out) = (refs[:4], refs[4:8]), refs[8:]
    z, y, x, c = place()
    share = out.shape[0]
    first = ((y * 2 + x) * 2 + c) * share
    mine = pl.ds(pl.multiple_of(first, share), share)
    groups = []
    planes = slot_planes(z)
    cols = out.shape[1] // 8
    for half, slots in zip(parts, ((0, 1, 2), (3,))):
        for k, slot in enumerate(slots):
            for part in range(2):
                col = (2 * planes[slot] + part) * cols
                where = pl.ds(pl.multiple_of(col, cols), cols)
                at = slice((2 * k + part) * cols, (2 * k + part + 1) * cols)
                own, from_x, from_y, from_xy = (ref[:, at].astype(F32) for ref in half)
                groups.append(
                    (where, own + from_x + (from_y + from_xy) + alpha_mix * hidden[mine, where].astype(F32))
                )
    width = out.shape[1]
    centre = sum(jnp.sum(g, axis=1, keepdims=True) for _, g in groups) / width
    spread = sum(jnp.sum(jnp.square(g - centre), axis=1, keepdims=True) for _, g in groups) / width
    factor = lax.rsqrt(spread + 1e-05)
    for where, g in groups:
        out[:, where] = ((g - centre) * factor * gain[:, where]).astype(BF)


def local_planes(
    query_one,
    query_two,
    key_one,
    key_two,
    values,
    mix_lambda,
    head_gain,
    stream,
    out_weight,
    first_gain,
    up_weight,
    down_weight,
    second_gain,
):
    tokens, w2 = query_one.shape
    qk = w2 // 2
    e = values.shape[1] // 2
    width = out_weight.shape[1]
    rows, half = up_weight.shape[0], up_weight.shape[1] // 2
    cols = down_weight.shape[1]

    def permute(value, move):
        pairs = []
        for z in range(4):
            for y in range(2):
                for x in range(2):
                    for c in range(2):
                        to = move(z, y, x, c)
                        if to is not None:
                            zz, yy, xx, cc = to
                            pairs.append(
                                (((z * 2 + y) * 2 + x) * 2 + c, ((zz * 2 + yy) * 2 + xx) * 2 + cc)
                            )
        return lax.ppermute(value, ("sp", "tp"), pairs)

    def across(value, dy, dx, dc):
        return permute(value, lambda z, y, x, c: (z, y ^ dy, x ^ dx, c ^ dc))

    def planes(block, dy=0):
        plus = permute(block, lambda z, y, x, c: (z + 1, y ^ dy, x, c) if z < 3 else None)
        minus = permute(block, lambda z, y, x, c: (z - 1, y ^ dy, x, c) if z > 0 else None)
        two = permute(block, lambda z, y, x, c: ((z + 2) % 4, y ^ dy, x, c))
        far = permute(two, lambda z, y, x, c: {1: (0, y, x, c), 2: (3, y, x, c)}.get(z))
        return block, plus, minus, two, far

    shards = (query_one, query_two, key_one, key_two, values, up_weight, down_weight)
    kv_own, kv_out, kvq_out, q_own, wt_own, wt_out = call(
        pack,
        [
            ((tokens, w2 + e), BF),
            ((tokens, w2 + e), BF),
            ((tokens, 2 * w2 + e), BF),
            ((tokens, w2), BF),
            ((2 * rows, half), BF),
            ((2 * rows, half), BF),
        ],
        shards,
        specs=[pl.BlockSpec(memory_space=pltpu.HBM)] * len(shards),
        scratch=[pltpu.VMEM(a.shape, a.dtype) for a in shards]
        + [pltpu.SemaphoreType.DMA((len(shards),))],
        vmem=60,
    )
    wo_x = across(out_weight, 0, 1, 0)
    kvs = [kv_own, across(kvq_out, 1, 0, 0)]
    kvs += planes(kv_own)[1:] + planes(kv_out, 1)[1:]
    wt_got = across(wt_out, 1, 0, 0)
    st_y = across(stream, 1, 0, 0)
    up_block, down_block = call(stack_weights, [((2, rows, half), BF)] * 2, (wt_own, wt_got))
    up_blocks, down_blocks = planes(up_block), planes(down_block)
    (st00,) = call(stack_rows, [((2 * tokens, stream.shape[1]), BF)], (stream, st_y))
    st10 = across(st00, 0, 1, 0)
    wo_c, wo_xc = across(out_weight, 0, 0, 1), across(wo_x, 0, 0, 1)
    st01, st11 = across(st00, 0, 0, 1), across(st10, 0, 0, 1)

    (att,) = call(
        functools.partial(attention, qk),
        [((2 * tokens, e), BF)],
        (mix_lambda, head_gain.reshape(1, -1), q_own, *kvs),
        specs=[SM] + [VM] * (2 + len(kvs)),
        scratch=[pltpu.VMEM((8 * tokens, w2 + e), BF)],
        flops=4 * 2 * tokens * tokens * 8 * (qk + e),
    )
    att_x = across(att, 0, 1, 0)
    att_y = across(att, 1, 0, 0)
    att_xy = across(att, 1, 1, 0)
    (heads0,) = call(merge_heads, [((2 * tokens, 4 * e), BF)], (att, att_x, att_y, att_xy))
    heads1 = across(heads0, 0, 0, 1)
    (hidden,) = call(
        norm_in,
        [((2 * tokens, width), BF)],
        (
            heads0,
            heads1,
            out_weight,
            wo_x,
            wo_c,
            wo_xc,
            st00,
            st10,
            st01,
            st11,
            first_gain.reshape(1, -1),
        ),
        flops=2 * 2 * tokens * width * 8 * e,
    )
    (act,) = call(
        mixer_up,
        [((2 * tokens, half), BF)],
        (hidden, *up_blocks),
        scratch=[pltpu.VMEM((8 * rows, half), BF)],
        flops=4 * tokens * width * half,
    )
    share = tokens // 4
    own, plus, minus, two, far = down_blocks
    pieces = []
    for body, args, slots in (
        (mixer_down_a, (act, own, plus, minus, two), 3), (mixer_down_b, (act, minus, far), 1)
    ):
        wide = slots * 2 * cols
        keep, send = call(
            body,
            [((4, share, wide), F32), ((4, share, wide), BF)],
            args,
            flops=4 * tokens * wide * half,
        )
        got = across(send, 0, 0, 1)
        mine, to_x, to_y, to_xy = call(
            pair_sum, [((share, wide), F32)] + [((share, wide), BF)] * 3, (keep, got)
        )
        pieces += [mine, across(to_x, 0, 1, 0), across(to_y, 1, 0, 0), across(to_xy, 1, 1, 0)]
    (out,) = call(norm_out, [((share, width), BF)], (*pieces, hidden, second_gain.reshape(1, -1)))
    return out


def solution(mesh):
    in_specs = (
        P("sp", "tp"),
        P("sp", "tp"),
        P("sp", "tp"),
        P("sp", "tp"),
        P("sp", "tp"),
        P("tp"),
        P(),
        P("sp", "tp"),
        P("tp", None),
        P(),
        P("sp", "tp"),
        P("tp", "sp"),
        P(),
    )
    out_specs = P(("sp", "tp"), None)
    planes = mesh.shape["sp"] == 8 and mesh.shape["tp"] == 4

    def local(*args):
        return (local_planes if planes else local_general)(*args)

    return jax.shard_map(local, mesh=mesh, in_specs=in_specs, out_specs=out_specs, check_vma=False)
```

```python
import functools
import math

import jax
import jax.numpy as jnp
from jax import lax
from jax.experimental import pallas as pl
from jax.experimental.pallas import tpu as pltpu
from jax.sharding import PartitionSpec as P


alpha_mix = 2.0**0.5
BF, F32 = jnp.bfloat16, jnp.float32


def layer_norm(value, gain):
    centre = jnp.mean(value, axis=-1, keepdims=True)
    spread = jnp.mean(jnp.square(value - centre), axis=-1, keepdims=True)
    return (value - centre) * lax.rsqrt(spread + 1e-05) * gain


def absorb_map(run_max, run_sum, run_acc, queries, keys, vals, scale):
    scores = jnp.einsum("qhd,khd->hqk", queries, keys, preferred_element_type=jnp.float32) * scale
    new_max = jnp.maximum(run_max, jnp.max(scores, axis=-1))
    factor = jnp.exp(run_max - new_max)
    expo = jnp.exp(scores - new_max[..., None])
    run_sum = run_sum * factor + jnp.sum(expo, axis=-1)
    run_acc = run_acc * factor[..., None] + jnp.einsum(
        "hqk,khe->hqe", expo.astype(jnp.bfloat16), vals, preferred_element_type=jnp.float32
    )
    return (new_max, run_sum, run_acc)


def local_general(
    query_one,
    query_two,
    key_one,
    key_two,
    values,
    mix_lambda,
    head_gain,
    stream,
    out_weight,
    first_gain,
    up_weight,
    down_weight,
    second_gain,
):
    tokens = query_one.shape[0]
    heads_local = mix_lambda.shape[0]
    qk_width = query_one.shape[1] // heads_local
    v_width = values.shape[1] // heads_local
    scale = qk_width ** (-0.5)
    queries_a = query_one.reshape(tokens, heads_local, qk_width)
    queries_b = query_two.reshape(tokens, heads_local, qk_width)
    lowest = jnp.full((heads_local, tokens), -1e30, jnp.float32)
    zero_sum = jnp.zeros((heads_local, tokens), jnp.float32)
    zero_acc = jnp.zeros((heads_local, tokens, v_width), jnp.float32)
    pieces = (
        lax.all_gather(key_one, "sp", axis=0, tiled=True),
        lax.all_gather(key_two, "sp", axis=0, tiled=True),
        lax.all_gather(values, "sp", axis=0, tiled=True),
    )
    count = pieces[0].shape[0]
    block = math.gcd(count, 1024)
    nblk = count // block
    keys_a = pieces[0].reshape(nblk, block, heads_local, qk_width)
    keys_b = pieces[1].reshape(nblk, block, heads_local, qk_width)
    vals = pieces[2].reshape(nblk, block, heads_local, v_width)

    def step(carry, inputs):
        max_a, sum_a, acc_a, max_b, sum_b, acc_b = carry
        max_a, sum_a, acc_a = absorb_map(
            max_a, sum_a, acc_a, queries_a, inputs[0], inputs[2], scale
        )
        max_b, sum_b, acc_b = absorb_map(
            max_b, sum_b, acc_b, queries_b, inputs[1], inputs[2], scale
        )
        return ((max_a, sum_a, acc_a, max_b, sum_b, acc_b), None)

    result, _ = lax.scan(
        step, (lowest, zero_sum, zero_acc, lowest, zero_sum, zero_acc), (keys_a, keys_b, vals)
    )
    _, sum_a, acc_a, _, sum_b, acc_b = result
    mixed = acc_a / sum_a[..., None] - mix_lambda[:, None, None] * acc_b / sum_b[..., None]
    normed = (
        mixed
        * lax.rsqrt(jnp.mean(jnp.square(mixed), axis=-1, keepdims=True) + 1e-05)
        * head_gain
        * 0.8
    )
    attended = jnp.transpose(normed.astype(jnp.bfloat16), (1, 0, 2)).reshape(
        tokens, heads_local * v_width
    )
    tp_index = lax.axis_index("tp")
    own_cols = stream.shape[1]
    col_start = tp_index * own_cols
    share = tokens // lax.axis_size("tp")
    row_start = tp_index * share
    partial_rows = jnp.dot(attended, out_weight, preferred_element_type=jnp.float32)
    own = lax.dynamic_slice_in_dim(partial_rows, col_start, own_cols, 1)
    own = own + alpha_mix * stream.astype(jnp.float32)
    pre = lax.psum(
        lax.dynamic_update_slice_in_dim(partial_rows, own, col_start, 1).astype(jnp.bfloat16), "tp"
    ).astype(jnp.float32)
    hidden_in = layer_norm(pre, first_gain).astype(jnp.bfloat16)
    up_full, down_full = (
        lax.all_gather(up_weight, "sp", axis=0, tiled=True),
        lax.all_gather(down_weight, "sp", axis=1, tiled=True),
    )
    upper = jnp.dot(hidden_in, up_full, preferred_element_type=jnp.float32)
    act = jnp.square(jax.nn.relu(upper)).astype(jnp.bfloat16)
    post = lax.psum_scatter(
        jnp.dot(act, down_full, preferred_element_type=jnp.float32).astype(jnp.bfloat16),
        "tp",
        scatter_dimension=0,
        tiled=True,
    ).astype(jnp.float32)
    post = post + alpha_mix * lax.dynamic_slice_in_dim(hidden_in, row_start, share, 0).astype(
        jnp.float32
    )
    return layer_norm(post, second_gain).astype(jnp.bfloat16)


VM = pl.BlockSpec(memory_space=pltpu.VMEM)
SM = pl.BlockSpec(memory_space=pltpu.SMEM)


def place():
    s, t = lax.axis_index("sp"), lax.axis_index("tp")
    return lax.div(s, 2), lax.rem(s, 2), lax.div(t, 2), lax.rem(t, 2)


def call(body, outs, args, specs=None, scratch=(), flops=0, vmem=24):
    outs = [jax.ShapeDtypeStruct(shape, kind) for shape, kind in outs]
    size = sum(a.size * a.dtype.itemsize for a in list(args) + outs)
    return pl.pallas_call(
        body,
        out_shape=outs,
        in_specs=specs or [VM] * len(args),
        out_specs=[VM] * len(outs),
        scratch_shapes=list(scratch),
        cost_estimate=pl.CostEstimate(flops=flops, bytes_accessed=size, transcendentals=0),
        compiler_params=pltpu.CompilerParams(vmem_limit_bytes=vmem * 2**20),
    )(*args)


def either(bit, emit):
    @pl.when(bit == 0)
    def _():
        emit(0)

    @pl.when(bit != 0)
    def _():
        emit(1)


def pack(q1, q2, k1, k2, v, down, st, *refs):
    kv_own, kvq_out, q_own, down_own, down_out = refs[:5]
    scratch = refs[5:]
    bufs, sems = scratch[:-1], scratch[-1]
    copies = [
        pltpu.make_async_copy(src, buf, sems.at[i])
        for i, (src, buf) in enumerate(zip((q1, q2, k1, k2, v, down, st), bufs))
    ]
    for copy in copies:
        copy.start()
    q1, q2, k1, k2, v, down, st = bufs
    _, y, _, _ = place()
    w, e = q1.shape[1] // 2, v.shape[1] // 2
    cols, part = down.shape[1], down_own.shape[0]
    half = 2 * part
    for copy in copies[:5]:
        copy.wait()

    def heads(bit):
        for head, dest in ((bit, kv_own), (1 - bit, kvq_out)):
            dest[:, :w] = k1[:, head * w : (head + 1) * w]
            dest[:, w : 2 * w] = k2[:, head * w : (head + 1) * w]
            dest[:, 2 * w : 2 * w + e] = v[:, head * e : (head + 1) * e]
        q_own[:, :w] = q1[:, bit * w : (bit + 1) * w]
        q_own[:, w:] = q2[:, bit * w : (bit + 1) * w]
        other, base = 1 - bit, 2 * w + e
        kvq_out[:, base : base + w] = q1[:, other * w : (other + 1) * w]
        kvq_out[:, base + w :] = q2[:, other * w : (other + 1) * w]

    def weights(bit):
        for side, to_down in ((bit, down_own), (1 - bit, down_out)):
            for k in range(2):
                first = side * half + k * part
                to_down[:part, k * cols : (k + 1) * cols] = down[first : first + part, :]

    either(y, heads)
    for copy in copies[5:]:
        copy.wait()
    either(y, weights)
    down_out[part:, :] = st[...]


def stack_down(own, got, st, down, rows2):
    part, tokens = own.shape[0], st.shape[0]
    down[0] = own[...]
    down[1] = got[:part, :]
    rows2[:tokens, :] = st[...]
    rows2[tokens:, :] = got[part:, :]


def stack_kv(own, got, out):
    tokens, wide = own.shape
    out[:tokens, :] = own[...]
    out[tokens:, :] = got[:, :wide]


def split_most(own, p1, m1, p2, m2, mine, theirs):
    z, y, _, _ = place()
    half = mine.shape[2]

    def emit(bit):
        for side, dest in ((bit, mine), (1 - bit, theirs)):
            where = slice(side * half, (side + 1) * half)
            for k, raw in enumerate((own, p1, m1)):
                dest[k] = raw[:, where]
            dest[3] = jnp.where(z < 2, m2[:, where], p2[:, where])

    either(y, emit)


def split_last(p3, m3, mine, theirs):
    z, y, _, _ = place()
    half = mine.shape[2]

    def emit(bit):
        for side, dest in ((bit, mine), (1 - bit, theirs)):
            where = slice(side * half, (side + 1) * half)
            dest[0] = jnp.where(z == 0, m3[:, where], p3[:, where])

    either(y, emit)


def stack_up(mine, got, *outs):
    for k, out in enumerate(outs):
        out[0] = mine[k]
        out[1] = got[k]


def attention(qk, lam, gain, q_own, kvq_y, own, p1, m1, p2, m2, p3, m3, att, full):
    z, y, _, _ = place()
    tokens = q_own.shape[0]
    blocks = (
        own[...],
        jnp.where(z < 2, m2[...], p2[...]),
        jnp.where(z == 0, m3[...], p1[...]),
        jnp.where(z == 3, p3[...], m1[...]),
    )
    for i, block in enumerate(blocks):
        full[i * 2 * tokens : (i + 1) * 2 * tokens, :] = block
    kvs = [full.at[i * tokens : (i + 1) * tokens, :] for i in range(8)]
    w2 = 2 * qk
    e = att.shape[1]
    rate = qk**-0.5 * math.log2(math.e)
    lane = lax.broadcasted_iota(jnp.int32, (tokens, w2), 1)
    weight = lam[y]
    for part in range(2):
        queries = (q_own[...] if part == 0 else kvq_y[:, w2 + e :]).astype(F32)
        outs = []
        for which in range(2):
            keep = (lane < qk) if which == 0 else (lane >= qk)
            masked = jnp.where(keep, queries, 0.0).astype(BF)
            tiles = [
                lax.dot_general(
                    masked, kv[:, :w2], (((1,), (1,)), ((), ())), preferred_element_type=F32
                )
                for kv in kvs
            ]
            top = functools.reduce(jnp.maximum, tiles)
            top = jnp.max(top, axis=1, keepdims=True)
            total, acc = None, None
            for tile, kv in zip(tiles, kvs):
                expo = jnp.exp2((tile - top) * rate)
                total = expo if total is None else total + expo
                part_acc = jnp.dot(
                    expo.astype(BF), kv[:, w2 : w2 + e], preferred_element_type=F32
                )
                acc = part_acc if acc is None else acc + part_acc
            outs.append(acc / jnp.sum(total, axis=1, keepdims=True))
        mixed = outs[0] - weight * outs[1]
        normed = (
            mixed
            * lax.rsqrt(jnp.mean(jnp.square(mixed), axis=-1, keepdims=True) + 1e-05)
            * gain[...]
            * 0.8
        )
        row = (y if part == 0 else 1 - y) * tokens
        att[pl.ds(pl.multiple_of(row, tokens), tokens), :] = normed.astype(BF)


def merge_heads(a, ax, ay, axy, out):
    _, y, _, _ = place()
    e = a.shape[1]

    def emit(bit):
        for dx, pair in enumerate(((a, ay), (ax, axy))):
            for dy in range(2):
                k = dx * 2 + (bit ^ dy)
                out[:, k * e : (k + 1) * e] = pair[dy][...]

    either(y, emit)


def norm_in(a0, a1, w00, w10, w01, w11, s00, s10, s01, s11, gain, hidden):
    _, y, x, c = place()
    rows = s00.shape[0] // 2
    cols = s00.shape[1]
    depth = w00.shape[0]
    for part in range(2):
        row = pl.multiple_of((y if part == 0 else 1 - y) * rows, rows)
        left = [a0[pl.ds(row, rows), :depth], a0[pl.ds(row, rows), depth:]]
        left += [a1[pl.ds(row, rows), :depth], a1[pl.ds(row, rows), depth:]]
        groups = []
        for dx, dc, st in ((0, 0, s00), (1, 0, s10), (0, 1, s01), (1, 1, s11)):
            col = ((x ^ dx) * 2 + (c ^ dc)) * cols
            where = pl.ds(pl.multiple_of(col, cols), cols)
            acc = alpha_mix * st[part * rows : (part + 1) * rows, :].astype(F32)
            for lhs, wt in zip(left, (w00, w10, w01, w11)):
                acc = acc + jnp.dot(lhs, wt[:, where], preferred_element_type=F32)
            groups.append((where, acc))
        width = cols * len(groups)
        centre = sum(jnp.sum(g, axis=1, keepdims=True) for _, g in groups) / width
        spread = (
            sum(jnp.sum(jnp.square(g - centre), axis=1, keepdims=True) for _, g in groups) / width
        )
        factor = lax.rsqrt(spread + 1e-05)
        for where, g in groups:
            hidden[pl.ds(row, rows), where] = ((g - centre) * factor * gain[:, where]).astype(BF)


def slots_of(own, p1, m1, two, far, z):
    return (
        own,
        two,
        lambda part: jnp.where(z == 0, m1(part), p1(part)),
        lambda part: jnp.where((z == 0) | (z == 3), far(part), m1(part)),
    )


def loads_of(*refs):
    return [lambda part, ref=ref: ref[part] for ref in refs]


def slot_planes(z):
    return z, lax.rem(z + 2, 4), jnp.where(z == 0, 1, z - 1), jnp.where(z == 0, 3, lax.rem(z + 1, 4))


def mixer_up(hidden, own, p1, m1, two, far, act, full):
    z, y, _, _ = place()
    rows = own.shape[1]
    for load, zz in zip(slots_of(*loads_of(own, p1, m1, two, far), z), slot_planes(z)):
        for part in range(2):
            first = (2 * zz + (y ^ part)) * rows
            full[pl.ds(pl.multiple_of(first, rows), rows), :] = load(part)
    upper = jnp.dot(hidden[...], full[...], preferred_element_type=F32)
    act[...] = jnp.square(jnp.maximum(upper, 0.0)).astype(BF)


def mixer_down(loads, act, keep, send):
    _, y, _, c = place()
    share = keep.shape[1]
    for slot, load in enumerate(loads):
        for part in range(2):
            block = load(part)
            cols = block.shape[1] // 2
            weight = jnp.concatenate([block[:, :cols], block[:, cols:]], axis=0)
            rows = jnp.dot(act[...], weight, preferred_element_type=F32)
            where = pl.ds(pl.multiple_of((2 * slot + (y ^ part)) * cols, cols), cols)

            def emit(bit, rows=rows, where=where):
                for k in range(keep.shape[0] * 2):
                    piece = rows[k * share : (k + 1) * share, :]
                    if k % 2 == bit:
                        keep[k // 2, :, where] = piece
                    else:
                        send[k // 2, :, where] = piece.astype(BF)

            either(c, emit)


def mixer_down_a(act, own, p1, m1, p2, m2, keep, send):
    z = place()[0]
    own, p1, m1 = loads_of(own, p1, m1)
    two = lambda part: jnp.where(z < 2, m2[part], p2[part])
    mixer_down(slots_of(own, p1, m1, two, None, z)[:3], act, keep, send)


def mixer_down_b(act, m1, p3, m3, keep, send):
    z = place()[0]
    far = lambda part: jnp.where(z == 0, m3[part], p3[part])
    mixer_down(slots_of(None, None, loads_of(m1)[0], None, far, z)[3:], act, keep, send)


def pair_sum(keep, got, own, to_x, to_y, to_xy):
    _, y, x, _ = place()

    def total(dy, dx):
        k = (y ^ dy) * 2 + (x ^ dx)
        return keep[k] + got[k].astype(F32)

    to_x[...] = total(0, 1).astype(BF)
    to_y[...] = total(1, 0).astype(BF)
    to_xy[...] = total(1, 1).astype(BF)
    own[...] = total(0, 0)


def norm_out(*refs):
    parts, (hidden, gain, out) = (refs[:4], refs[4:8]), refs[8:]
    z, y, x, c = place()
    share = out.shape[0]
    first = ((y * 2 + x) * 2 + c) * share
    mine = pl.ds(pl.multiple_of(first, share), share)
    groups = []
    planes = slot_planes(z)
    cols = out.shape[1] // 8
    for half, slots in zip(parts, ((0, 1, 2), (3,))):
        for k, slot in enumerate(slots):
            for part in range(2):
                col = (2 * planes[slot] + part) * cols
                where = pl.ds(pl.multiple_of(col, cols), cols)
                at = slice((2 * k + part) * cols, (2 * k + part + 1) * cols)
                own, from_x, from_y, from_xy = (ref[:, at].astype(F32) for ref in half)
                groups.append(
                    (where, own + from_x + (from_y + from_xy) + alpha_mix * hidden[mine, where].astype(F32))
                )
    width = out.shape[1]
    centre = sum(jnp.sum(g, axis=1, keepdims=True) for _, g in groups) / width
    spread = sum(jnp.sum(jnp.square(g - centre), axis=1, keepdims=True) for _, g in groups) / width
    factor = lax.rsqrt(spread + 1e-05)
    for where, g in groups:
        out[:, where] = ((g - centre) * factor * gain[:, where]).astype(BF)


def local_planes(
    query_one,
    query_two,
    key_one,
    key_two,
    values,
    mix_lambda,
    head_gain,
    stream,
    out_weight,
    first_gain,
    up_weight,
    down_weight,
    second_gain,
):
    tokens, w2 = query_one.shape
    qk = w2 // 2
    e = values.shape[1] // 2
    width = out_weight.shape[1]
    rows, half = up_weight.shape[0], up_weight.shape[1] // 2
    cols = down_weight.shape[1]

    def permute(value, move):
        pairs = []
        for z in range(4):
            for y in range(2):
                for x in range(2):
                    for c in range(2):
                        to = move(z, y, x, c)
                        if to is not None:
                            zz, yy, xx, cc = to
                            pairs.append(
                                (((z * 2 + y) * 2 + x) * 2 + c, ((zz * 2 + yy) * 2 + xx) * 2 + cc)
                            )
        return lax.ppermute(value, ("sp", "tp"), pairs)

    def across(value, dy, dx, dc):
        return permute(value, lambda z, y, x, c: (z, y ^ dy, x ^ dx, c ^ dc))

    def planes(block):
        got = [block]
        up = down = block
        for hop in range(1, 4):
            up = permute(up, lambda z, y, x, c: (z + 1, y, x, c) if hop - 1 <= z < 3 else None)
            down = permute(down, lambda z, y, x, c: (z - 1, y, x, c) if 0 < z <= 4 - hop else None)
            got += [up, down]
        return got

    _, raw_p1, raw_m1, raw_p2, raw_m2, raw_p3, raw_m3 = planes(up_weight)
    shards = (query_one, query_two, key_one, key_two, values, down_weight, stream)
    part = half // 2
    kv_own, kvq_out, q_own, down_own, down_out = call(
        pack,
        [
            ((tokens, w2 + e), BF),
            ((tokens, 2 * w2 + e), BF),
            ((tokens, w2), BF),
            ((part, half), BF),
            ((part + tokens, half), BF),
        ],
        shards,
        specs=[pl.BlockSpec(memory_space=pltpu.HBM)] * len(shards),
        scratch=[pltpu.VMEM(a.shape, a.dtype) for a in shards]
        + [pltpu.SemaphoreType.DMA((len(shards),))],
        vmem=60,
    )
    wo_x = across(out_weight, 0, 1, 0)
    kvq_y = across(kvq_out, 1, 0, 0)
    (kv_block,) = call(stack_kv, [((2 * tokens, w2 + e), BF)], (kv_own, kvq_y))
    kvs = planes(kv_block)
    down_got = across(down_out, 1, 0, 0)
    down_block, st00 = call(
        stack_down, [((2, part, half), BF), ((2 * tokens, half), BF)], (down_own, down_got, stream)
    )

    def up_of(body, raws, count):
        mine, theirs = call(body, [((count, rows, half), BF)] * 2, raws)
        got = across(theirs, 1, 0, 0)
        return call(stack_up, [((2, rows, half), BF)] * count, (mine, got))

    raws = (up_weight, raw_p1, raw_m1, raw_p2, raw_m2)
    up_blocks = [*up_of(split_most, raws, 4), *up_of(split_last, (raw_p3, raw_m3), 1)]
    down_blocks = planes(down_block)
    st10 = across(st00, 0, 1, 0)
    wo_c, wo_xc = across(out_weight, 0, 0, 1), across(wo_x, 0, 0, 1)
    st01, st11 = across(st00, 0, 0, 1), across(st10, 0, 0, 1)

    (att,) = call(
        functools.partial(attention, qk),
        [((2 * tokens, e), BF)],
        (mix_lambda, head_gain.reshape(1, -1), q_own, kvq_y, *kvs),
        specs=[SM] + [VM] * (3 + len(kvs)),
        scratch=[pltpu.VMEM((8 * tokens, w2 + e), BF)],
        flops=4 * 2 * tokens * tokens * 8 * (qk + e),
    )
    att_x = across(att, 0, 1, 0)
    att_y = across(att, 1, 0, 0)
    att_xy = across(att, 1, 1, 0)
    (heads0,) = call(merge_heads, [((2 * tokens, 4 * e), BF)], (att, att_x, att_y, att_xy))
    heads1 = across(heads0, 0, 0, 1)
    (hidden,) = call(
        norm_in,
        [((2 * tokens, width), BF)],
        (
            heads0,
            heads1,
            out_weight,
            wo_x,
            wo_c,
            wo_xc,
            st00,
            st10,
            st01,
            st11,
            first_gain.reshape(1, -1),
        ),
        flops=2 * 2 * tokens * width * 8 * e,
    )
    (act,) = call(
        mixer_up,
        [((2 * tokens, half), BF)],
        (hidden, *up_blocks),
        scratch=[pltpu.VMEM((8 * rows, half), BF)],
        flops=4 * tokens * width * half,
    )
    share = tokens // 4
    own, p1, m1, p2, m2, p3, m3 = down_blocks
    pieces = []
    for body, args, slots in (
        (mixer_down_a, (act, own, p1, m1, p2, m2), 3), (mixer_down_b, (act, m1, p3, m3), 1)
    ):
        wide = slots * 2 * cols
        keep, send = call(
            body,
            [((4, share, wide), F32), ((4, share, wide), BF)],
            args,
            flops=4 * tokens * wide * half,
        )
        got = across(send, 0, 0, 1)
        mine, to_x, to_y, to_xy = call(
            pair_sum, [((share, wide), F32)] + [((share, wide), BF)] * 3, (keep, got)
        )
        pieces += [mine, across(to_x, 0, 1, 0), across(to_y, 1, 0, 0), across(to_xy, 1, 1, 0)]
    (out,) = call(norm_out, [((share, width), BF)], (*pieces, hidden, second_gain.reshape(1, -1)))
    return out


def solution(mesh):
    in_specs = (
        P("sp", "tp"),
        P("sp", "tp"),
        P("sp", "tp"),
        P("sp", "tp"),
        P("sp", "tp"),
        P("tp"),
        P(),
        P("sp", "tp"),
        P("tp", None),
        P(),
        P("sp", "tp"),
        P("tp", "sp"),
        P(),
    )
    out_specs = P(("sp", "tp"), None)
    planes = mesh.shape["sp"] == 8 and mesh.shape["tp"] == 4

    def local(*args):
        return (local_planes if planes else local_general)(*args)

    return jax.shard_map(local, mesh=mesh, in_specs=in_specs, out_specs=out_specs, check_vma=False)
```
